32 devices in a mesh: sp: 8 (over z, y), tp: 4 (over x, core).
Axes of the slice: x: 2, y: 2, z: 4, core: 2. Of those that a mesh axis runs over, the one named last changes fastest.
Arguments:
- stream: bfloat16 [2048, 2048], P('sp', 'tp'), may hold values from -6 to 6
- norm_gain: float32 [2, 2048], replicated, may hold values from 0.1 to 1.9
- w_value: bfloat16 [2, 2048, 1024], P(None, 'sp', 'tp'), may hold values from -0.125 to 0.125
- w_gate: bfloat16 [2, 2048, 1024], P(None, 'sp', 'tp'), may hold values from -0.125 to 0.125
- conv_taps: float32 [2, 128, 1024], P(None, None, 'tp'), as said below
- channel_gain: float32 [2, 1024], P(None, 'tp'), may hold values from 0.1 to 1.9
- w_out: bfloat16 [2, 1024, 2048], P(None, 'tp', 'sp'), may hold values from -0.1875 to 0.1875
Outputs:
- result: bfloat16 [2048, 2048], P('sp', 'tp')
The draws below stay inside these ranges and needn't reach their ends.
Inputs may be any that keep to these rules, and one draw needn't show every extreme that they name: `conv_taps`: taps of each block of 128 consecutive channels share a scale factor of its own.
All inputs are finite; a program needn't handle non-finite values.
Results may differ from the reference program's by a relative error of at most 0.012.
Values may be sent and summed in bfloat16 or wider, within the bound.
A program may use at most 64 MiB of HBM per device.

```python
import jax
import jax.numpy as jnp
from jax import lax

D = 2048
C = 1024
KW = 128
LAYERS = 2
TOKENS = 2048


def draw_conv_taps(key, part):
    first, second = jax.random.split(key)
    base = jax.random.normal(first, (LAYERS, KW, 8, C // 8), jnp.float32)
    scales = jnp.exp(jax.random.uniform(second, (LAYERS, 1, 8, 1), jnp.float32, -1.2039728, 1.0986123))
    taps = base * scales * KW ** (-0.5)
    return taps.reshape(LAYERS, KW, C).astype(jnp.float32)


def shard_levels(key, dims, pieces, least, high):
    level, own = 1.0, jax.random.fold_in(key, 6)
    for axis_at, blocks in pieces:
        draws = jnp.exp(jax.random.uniform(jax.random.fold_in(own, axis_at), (blocks,), jnp.float32, least / len(pieces), high / len(pieces)))
        level = level * jnp.repeat(draws, dims[axis_at] // blocks).reshape([-1 if axis == axis_at else 1 for axis in range(len(dims))])
    return level


def normal_values(key, extent, scale, limit, cuts=(), held_as=jnp.bfloat16):
    factor_of = shard_levels(key, extent, cuts, -0.22, 0.18) if cuts else 1.0
    values = jax.random.normal(key, extent, jnp.float32) * scale * factor_of
    return jnp.minimum(jnp.maximum(values, -limit), limit).astype(held_as)


def setup_inputs(seed: int = 0) -> dict:
    key_list = jax.random.split(jax.random.key(seed), 8)
    stream = normal_values(key_list[0], (TOKENS, D), 1.0, 6.0, ((0, 8), (1, 4)))
    norm_gain = jnp.clip(1.0 + 0.18 * jax.random.normal(key_list[1], (LAYERS, D), jnp.float32), 0.1, 1.9)
    w_value = normal_values(key_list[2], (LAYERS, D, C), D ** -0.5, 0.125, ((1, 8), (2, 4)))
    w_gate = normal_values(key_list[3], (LAYERS, D, C), D ** -0.5, 0.125, ((1, 8), (2, 4)))
    conv_taps = draw_conv_taps(jax.random.fold_in(key_list[7], 71), 0)
    channel_gain = jnp.clip(1.0 + 0.18 * jax.random.normal(key_list[5], (LAYERS, C), jnp.float32), 0.1, 1.9)
    w_out = normal_values(key_list[6], (LAYERS, C, D), C ** -0.5, 0.1875, ((1, 4), (2, 8)))
    return {"stream": stream, "norm_gain": norm_gain, "w_value": w_value, "w_gate": w_gate, "conv_taps": conv_taps, "channel_gain": channel_gain, "w_out": w_out}


def causal_conv(glu, taps):
    padded = jnp.concatenate([jnp.zeros((KW - 1, C), jnp.float32), glu.astype(jnp.float32)], axis=0)

    def add_tap(index, total):
        offset = jnp.asarray(index).astype(jnp.int32)
        window = lax.dynamic_slice_in_dim(padded, offset, TOKENS, 0)
        row = lax.dynamic_slice_in_dim(taps, offset, 1, 0)
        return total + window * row
    return lax.fori_loop(0, KW, add_tap, jnp.zeros((TOKENS, C), jnp.float32))

def reference(stream, norm_gain, w_value, w_gate, conv_taps, channel_gain, w_out):
    x = stream
    for layer in range(LAYERS):
        xf = x.astype(jnp.float32)
        normed = (xf * lax.rsqrt(lax.optimization_barrier(jnp.mean(xf * xf, axis=1, keepdims=True)) + 1e-06) * norm_gain[layer]).astype(jnp.bfloat16)
        value = jnp.dot(normed, w_value[layer], preferred_element_type=jnp.float32)
        gate = jnp.dot(normed, w_gate[layer], preferred_element_type=jnp.float32)
        glu = (value * jax.nn.sigmoid(gate)).astype(jnp.bfloat16)
        conv = causal_conv(glu, conv_taps[layer])
        mean = lax.optimization_barrier(jnp.mean(conv, axis=1, keepdims=True))
        centred = conv - mean
        spread = lax.optimization_barrier(jnp.mean(centred * centred, axis=1, keepdims=True))
        act = jax.nn.silu(centred * lax.rsqrt(spread + 1e-05) * channel_gain[layer]).astype(jnp.bfloat16)
        branch = jnp.dot(act, w_out[layer], preferred_element_type=jnp.float32)
        x = (xf + branch).astype(jnp.bfloat16)
    return x
```

```python
import functools

import jax
import jax.numpy as jnp
from jax import lax
from jax.experimental import pallas as pl
from jax.experimental.pallas import tpu as pltpu
from jax.sharding import PartitionSpec as P

F32, BF16 = jnp.float32, jnp.bfloat16
LANES = 128
ROW_TILE = 16
MESH = pl.DeviceIdType.MESH


def span(masks):
    found = [0]
    for mask in masks:
        found = found + [entry ^ mask for entry in found]
    return found


def parts_of(rows, most):
    parts = most
    while rows % (parts * ROW_TILE):
        parts //= 2
    return parts


def ring_chunks(layers, rows, width):
    stages = []
    for layer in range(layers):
        parts = parts_of(rows, 4)
        step = rows // parts
        stages.append(
            [(which, layer, which, part * step, step, 0, width) for part in range(parts) for which in (0, 1)]
        )
        parts = parts_of(rows, 2)
        step, half = rows // parts, width // 2
        stages.append(
            [(2, layer, way, part * step, step, way * half, half) for part in range(parts) for way in (0, 1)]
        )
    return stages


def kernel(
    count, peers, stages,
    x_ref, gain_ref, wv_ref, wg_ref, taps_ref, channel_ref, wo_ref, out_ref,
    full, gathered, normed, glu, halo, padded, conv, stat, act, mine, leaving, landing, middle,
    ring_send, ring_recv, x_send, x_recv, halo_send, halo_recv, stat_send, stat_recv, sum_send, sum_recv, own_sem,
):
    s, t = lax.axis_index("sp"), lax.axis_index("tp")
    tokens, part = x_ref.shape
    layers, rows, width = wv_ref.shape
    features = rows * count
    taps = taps_ref.shape[1]
    channels = width * peers
    groups = width // LANES
    last = count - 1
    lag = last // 2

    odd = s % 2
    place = (1 - odd) * (s // 2) + odd * (last - s // 2)

    def at_place(where):
        where = (where + count) % count
        upper = where // (count // 2)
        return (1 - upper) * (2 * where) + upper * (2 * (last - where) + 1)

    ahead, behind = at_place(place + 1), at_place(place - 1)
    masks = []
    mask = peers // 2
    while mask:
        masks.append(mask)
        mask //= 2

    def partner(bits):
        other = t
        for mask in masks:
            if bits & mask:
                other = other + mask - 2 * mask * ((t // mask) % 2)
        return other

    after, before = (s + 1) % count, (s + last) % count
    barrier = pltpu.get_barrier_semaphore()
    greeted = [(ahead, t), (behind, t), (after, t), (before, t)]
    greeted += [(s, partner(bits)) for bits in range(1, peers)]
    for who in greeted:
        pl.semaphore_signal(barrier, inc=1, device_id=who, device_id_type=MESH)
    pl.semaphore_wait(barrier, len(greeted))

    sources = (wv_ref, wg_ref, wo_ref)
    own_copies = []
    for which in range(3):
        own = pltpu.make_async_copy(
            sources[which],
            full.at[which, :, pl.ds(pl.multiple_of(s * rows, rows), rows), :],
            own_sem.at[which],
        )
        own.start()
        own_copies.append(own)

    numbered, total = [], 0
    for stage in stages:
        numbered.append([(total + offset, piece) for offset, piece in enumerate(stage)])
        total += len(stage)

    def ring_copy(number, piece, step, first, recv_step):
        which, layer, way, row, height, lane, lanes = piece
        block = at_place(place - step) if way == 0 else at_place(place + step)
        lane_slice = pl.ds(lane, lanes)
        start = pl.multiple_of(block * rows + row, ROW_TILE)
        there = full.at[which, layer, pl.ds(start, height), lane_slice]
        here = sources[which].at[layer, pl.ds(row, height), lane_slice] if first else there
        return pltpu.make_async_remote_copy(
            src_ref=here,
            dst_ref=there,
            send_sem=ring_send.at[number, step],
            recv_sem=ring_recv.at[number, recv_step],
            device_id=((ahead, behind)[way], t),
            device_id_type=MESH,
        )

    offsets = [layer * last + extra for layer in range(layers) for extra in (0, lag)]
    edges = sorted({offset + extra for offset in offsets for extra in (0, 1, last, last + 1)})
    clock = [0]

    def advance(to):
        while clock[0] < to:
            now = clock[0]
            end = min([edge for edge in edges if edge > now] + [to])
            end = min(end, to)
            active = [
                (stage, offset, now - offset)
                for stage, offset in zip(numbered, offsets)
                if 0 <= now - offset <= last
            ]

            def slot(at):
                for stage, offset, shown in active:
                    step = at - offset
                    for number, piece in stage:
                        if shown == 0:
                            ring_copy(number, piece, 0, True, 0).start()
                            continue
                        if shown == last:
                            which, layer, way, row, height, lane, lanes = piece
                            ring_copy(number, piece, last - 1, False, last - 1).wait_recv()
                            continue
                        ring_copy(number, piece, step, False, step - 1).wait_recv()
                        ring_copy(number, piece, step, False, step).start()

            if end - now == 1:
                slot(now)
            else:
                def body(at, carry):
                    slot(at)
                    return carry

                lax.fori_loop(now, end, body, 0)
            clock[0] = end

    def share_copy(layer, source, mask, sub):
        return pltpu.make_async_remote_copy(
            src_ref=source,
            dst_ref=gathered.at[layer, partner(sub)],
            send_sem=x_send.at[layer, mask ^ sub],
            recv_sem=x_recv.at[layer, mask ^ sub],
            device_id=(s, partner(mask)),
            device_id_type=MESH,
        )

    order = [(mask, sub) for place_, mask in enumerate(masks) for sub in span(masks[:place_])]

    def share_start(layer, source):
        for mask in masks:
            share_copy(layer, source, mask, 0).start()
        gathered[layer, t] = source[...]

    def share_relay(layer, source):
        for mask, sub in order:
            if sub:
                got = gathered.at[layer, partner(sub)]
                share_copy(layer, got, mask, sub).start()
            share_copy(layer, source, mask, sub).wait_recv()

    def share_end(layer, source):
        for mask, sub in order:
            share_copy(layer, source, mask, sub).wait_send()

    def normalise(layer):
        squares = jnp.zeros((tokens, 1), F32)
        for block in range(peers):
            value = gathered[layer, block].astype(F32)
            squares += jnp.sum(value * value, axis=1, keepdims=True)
        scale = lax.rsqrt(squares / features + 1e-06)
        for block in range(peers):
            gain = gain_ref[layer : layer + 1, block * part : (block + 1) * part]
            normed[:, block * part : (block + 1) * part] = (
                gathered[layer, block].astype(F32) * scale * gain
            ).astype(BF16)

    def halo_copy(layer):
        return pltpu.make_async_remote_copy(
            src_ref=glu.at[layer, pl.ds(tokens - taps, taps), :],
            dst_ref=halo.at[layer],
            send_sem=halo_send.at[layer],
            recv_sem=halo_recv.at[layer],
            device_id=(after, t),
            device_id_type=MESH,
        )

    def gated(layer):
        value = jnp.dot(normed[...], full[0, layer], preferred_element_type=F32)
        gate = jnp.dot(normed[...], full[1, layer], preferred_element_type=F32)
        rounded = (value * jax.nn.sigmoid(gate)).astype(BF16)
        glu[layer] = rounded

        @pl.when(s < last)
        def _():
            halo_copy(layer).start()

        wide = rounded.astype(F32)
        for group in range(groups):
            padded[group, taps:, :] = wide[:, group * LANES : (group + 1) * LANES]

    def halo_arrive(layer):
        @pl.when(s > 0)
        def _():
            halo_copy(layer).wait_recv()
            wide = halo[layer].astype(F32)
            for group in range(groups):
                padded[group, :taps, :] = wide[:, group * LANES : (group + 1) * LANES]

        @pl.when(s == 0)
        def _():
            padded[:, :taps, :] = jnp.zeros((groups, taps, LANES), F32)

    half = tokens // 2

    def convolve(layer, which):
        for group in range(groups):
            lanes = slice(group * LANES, (group + 1) * LANES)

            def body(block, total, group=group, lanes=lanes):
                eight = taps_ref[layer, pl.ds(pl.multiple_of(block * 8, 8), 8), lanes]
                for unit in range(8):
                    total += eight[unit : unit + 1] * padded[group, pl.ds(which * half + block * 8 + unit + 1, half), :]
                return total

            conv[which * half : (which + 1) * half, lanes] = lax.fori_loop(
                0, taps // 8, body, jnp.zeros((half, LANES), F32)
            )

    def stat_copy(layer, bits):
        return pltpu.make_async_remote_copy(
            src_ref=stat.at[layer, t],
            dst_ref=stat.at[layer, t],
            send_sem=stat_send.at[layer, bits],
            recv_sem=stat_recv.at[layer, bits],
            device_id=(s, partner(bits)),
            device_id_type=MESH,
        )

    def stat_start(layer):
        value = conv[...]
        sums = jnp.sum(value, axis=1, keepdims=True)
        centred = value - sums / width
        squares = jnp.sum(centred * centred, axis=1, keepdims=True)
        lane = lax.broadcasted_iota(jnp.int32, (tokens, LANES), 1)
        packed = jnp.where(lane == 0, sums, jnp.where(lane == 1, squares, 0.0))
        stat[layer, t] = packed.T[:8, :]
        for bits in range(1, peers):
            stat_copy(layer, bits).start()

    def activate(layer):
        for bits in range(1, peers):
            stat_copy(layer, bits).wait_recv()
        every = [stat[layer, block] for block in range(peers)]
        mean = sum(entry[0:1] for entry in every) / channels
        squares = sum(
            entry[1:2] + width * (entry[0:1] / width - mean) * (entry[0:1] / width - mean) for entry in every
        )
        scale = lax.rsqrt(squares / channels + 1e-05)
        row = lax.broadcasted_iota(jnp.int32, (LANES, tokens), 0)
        columns = jnp.where(row == 0, mean, jnp.where(row == 1, scale, 0.0)).T
        v = (conv[...] - columns[:, 0:1]) * columns[:, 1:2] * channel_ref[layer : layer + 1, :]
        act[...] = (v * jax.nn.sigmoid(v)).astype(BF16)

    def sum_copy(layer, mask, sub):
        return pltpu.make_async_remote_copy(
            src_ref=leaving.at[layer, mask ^ sub],
            dst_ref=landing.at[layer, mask ^ sub],
            send_sem=sum_send.at[layer, mask ^ sub],
            recv_sem=sum_recv.at[layer, mask ^ sub],
            device_id=(s, partner(mask)),
            device_id_type=MESH,
        )

    rising = masks[::-1]

    def product(layer, bits):
        start = pl.multiple_of(partner(bits) * part, part)
        return lax.dot_general(
            act[...],
            full[2, layer, pl.ds(start, part), :],
            (((1,), (1,)), ((), ())),
            preferred_element_type=F32,
        )

    def reduce_start(layer):
        mask = rising[0]
        subs = span(rising[1:])[::-1]
        for sub in subs:
            leaving[layer, mask ^ sub] = product(layer, mask ^ sub).astype(BF16)
            sum_copy(layer, mask, sub).start()
        for sub in subs:
            mine[sub] = product(layer, sub)
            sum_copy(layer, mask, sub).wait_recv()
            mine[sub] = mine[sub] + landing[layer, mask ^ sub].astype(F32)
            if len(rising) > 1 and sub & rising[1]:
                leaving[layer, sub] = mine[sub].astype(BF16)
                sum_copy(layer, rising[1], sub ^ rising[1]).start()

    def reduce_end(layer, source, target):
        for level in range(1, len(rising)):
            mask = rising[level]
            for sub in span(rising[level + 1 :])[::-1]:
                sum_copy(layer, mask, sub).wait_recv()
                mine[sub] = mine[sub] + landing[layer, mask ^ sub].astype(F32)
                if level + 1 < len(rising) and sub & rising[level + 1]:
                    leaving[layer, sub] = mine[sub].astype(BF16)
                    sum_copy(layer, rising[level + 1], sub ^ rising[level + 1]).start()
        target[...] = (source[...].astype(F32) + mine[0]).astype(BF16)

    current = x_ref
    share_start(0, current)
    advance(min(3, last))
    share_relay(0, current)
    advance(min(4, last))
    normalise(0)
    for layer in range(layers):
        base = (layer + 1) * last
        if layer == 0:
            for own in own_copies:
                own.wait()
        advance(base + 1)
        gated(layer)
        advance(base + 2)
        halo_arrive(layer)
        convolve(layer, 0)
        advance(base + min(3, lag))
        convolve(layer, 1)
        stat_start(layer)
        advance(base + lag + 1)
        activate(layer)
        reduce_start(layer)
        if layer + 1 < layers:
            advance(base + lag + 2)
            reduce_end(layer, current, middle.at[layer])
            current = middle.at[layer]
            share_start(layer + 1, current)
            advance(base + lag + 3)
            share_relay(layer + 1, current)
            normalise(layer + 1)
        else:
            reduce_end(layer, current, out_ref)

    for layer in range(layers):
        source = x_ref if layer == 0 else middle.at[layer - 1]
        share_end(layer, source)
        for bits in range(1, peers):
            stat_copy(layer, bits).wait_send()
        for level, mask in enumerate(rising):
            for sub in span(rising[level + 1 :]):
                sum_copy(layer, mask, sub).wait_send()

        @pl.when(s < last)
        def _(layer=layer):
            halo_copy(layer).wait_send()

    def drain(step, carry):
        for stage in numbered:
            for number, piece in stage:
                ring_copy(number, piece, step, False, step).wait_send()
        return carry

    lax.fori_loop(0, last, drain, 0)


def shards(count, peers, stream, norm_gain, w_value, w_gate, conv_taps, channel_gain, w_out):
    tokens, part = stream.shape
    layers, rows, width = w_value.shape
    taps = conv_taps.shape[1]
    features = rows * count
    stages = ring_chunks(layers, rows, width)
    pieces = sum(len(stage) for stage in stages)
    dma = pltpu.SemaphoreType.DMA
    return pl.pallas_call(
        functools.partial(kernel, count, peers, stages),
        out_shape=jax.ShapeDtypeStruct((tokens, part), BF16),
        in_specs=[pl.BlockSpec(memory_space=pltpu.VMEM)] * 7,
        out_specs=pl.BlockSpec(memory_space=pltpu.VMEM),
        scratch_shapes=[
            pltpu.VMEM((3, layers, features, width), BF16),
            pltpu.VMEM((layers, peers, tokens, part), BF16),
            pltpu.VMEM((tokens, features), BF16),
            pltpu.VMEM((layers, tokens, width), BF16),
            pltpu.VMEM((layers, taps, width), BF16),
            pltpu.VMEM((width // LANES, taps + tokens, LANES), F32),
            pltpu.VMEM((tokens, width), F32),
            pltpu.VMEM((layers, peers, 8, tokens), F32),
            pltpu.VMEM((tokens, width), BF16),
            pltpu.VMEM((peers, tokens, part), F32),
            pltpu.VMEM((layers, peers, tokens, part), BF16),
            pltpu.VMEM((layers, peers, tokens, part), BF16),
            pltpu.VMEM((layers, tokens, part), BF16),
            dma((pieces, count - 1)),
            dma((pieces, count - 1)),
            dma((layers, peers)),
            dma((layers, peers)),
            dma((layers,)),
            dma((layers,)),
            dma((layers, peers)),
            dma((layers, peers)),
            dma((layers, peers)),
            dma((layers, peers)),
            dma((3,)),
        ],
        compiler_params=pltpu.CompilerParams(
            collective_id=0, has_side_effects=True, vmem_limit_bytes=60 * 1024 * 1024
        ),
    )(stream, norm_gain, w_value, w_gate, conv_taps, channel_gain, jnp.swapaxes(w_out, 1, 2))


def solution(mesh):
    return jax.shard_map(
        functools.partial(shards, mesh.shape["sp"], mesh.shape["tp"]),
        mesh=mesh,
        in_specs=(
            P("sp", "tp"),
            P(),
            P(None, "sp", "tp"),
            P(None, "sp", "tp"),
            P(None, None, "tp"),
            P(None, "tp"),
            P(None, "tp", "sp"),
        ),
        out_specs=P("sp", "tp"),
        check_vma=False,
    )
```

```python
import functools

import jax
import jax.numpy as jnp
from jax import lax
from jax.experimental import pallas as pl
from jax.experimental.pallas import tpu as pltpu
from jax.sharding import PartitionSpec as P

F32, BF16 = jnp.float32, jnp.bfloat16
LANES = 128
ROW_TILE = 16
MESH = pl.DeviceIdType.MESH
PLAN = (3, 0, 3, 1, 2, 2, 2)


def span(masks):
    found = [0]
    for mask in masks:
        found = found + [entry ^ mask for entry in found]
    return found


def parts_of(rows, most):
    parts = most
    while rows % (parts * ROW_TILE):
        parts //= 2
    return parts


def ring_chunks(layers, rows, width, columns):
    stages = []
    for layer in range(layers):
        parts = parts_of(rows, 4)
        step = rows // parts
        stages.append(
            [(which, layer, which, part * step, step, 0, width) for part in range(parts) for which in (0, 1)]
        )
        parts = parts_of(width, 4) if columns % LANES == 0 else 2
        high, step = (width // parts, columns) if columns % LANES == 0 else (rows, width // parts)
        stages.append(
            [
                (2, layer, part % 2, part * high, high, 0, step)
                if columns % LANES == 0
                else (2, layer, part % 2, 0, high, part * step, step)
                for part in range(parts)
            ]
        )
    return stages


def kernel(
    count, peers, stages,
    x_ref, gain_ref, wv_ref, wg_ref, taps_ref, channel_ref, wo_ref, out_ref,
    full, full_out, gathered, normed, glu, halo, padded, conv, stat, act, mine, leaving, landing, middle,
    ring_send, ring_recv, x_send, x_recv, halo_send, halo_recv, stat_send, stat_recv, sum_send, sum_recv, own_sem,
):
    s, t = lax.axis_index("sp"), lax.axis_index("tp")
    tokens, part = x_ref.shape
    layers, rows, width = wv_ref.shape
    features = rows * count
    taps = taps_ref.shape[1]
    channels = width * peers
    groups = width // LANES
    last = count - 1

    odd = s % 2
    place = (1 - odd) * (s // 2) + odd * (last - s // 2)

    def at_place(where):
        where = (where + count) % count
        upper = where // (count // 2)
        return (1 - upper) * (2 * where) + upper * (2 * (last - where) + 1)

    ahead, behind = at_place(place + 1), at_place(place - 1)
    masks = []
    mask = peers // 2
    while mask:
        masks.append(mask)
        mask //= 2

    def partner(bits):
        other = t
        for mask in masks:
            if bits & mask:
                other = other + mask - 2 * mask * ((t // mask) % 2)
        return other

    after, before = (s + 1) % count, (s + last) % count
    barrier = pltpu.get_barrier_semaphore()
    greeted = [(ahead, t), (behind, t), (after, t), (before, t)]
    greeted += [(s, partner(bits)) for bits in range(1, peers)]
    for who in greeted:
        pl.semaphore_signal(barrier, inc=1, device_id=who, device_id_type=MESH)
    pl.semaphore_wait(barrier, len(greeted))

    sources = (wv_ref, wg_ref, wo_ref)
    own_copies = []
    for which in range(3):
        own_place = full.at[which, :, pl.ds(pl.multiple_of(s * rows, rows), rows), :] if which < 2 else full_out.at[:, s]
        own = pltpu.make_async_copy(sources[which], own_place, own_sem.at[which])
        own.start()
        own_copies.append(own)

    numbered, total = [], 0
    for stage in stages:
        numbered.append([(total + offset, piece) for offset, piece in enumerate(stage)])
        total += len(stage)

    def ring_copy(number, piece, step, first, recv_step):
        which, layer, way, row, height, lane, lanes = piece
        block = at_place(place - step) if way == 0 else at_place(place + step)
        lane_slice = pl.ds(lane, lanes)
        if which < 2:
            start = pl.multiple_of(block * rows + row, ROW_TILE)
            there = full.at[which, layer, pl.ds(start, height), lane_slice]
        else:
            there = full_out.at[layer, block, pl.ds(row, height), lane_slice]
        here = sources[which].at[layer, pl.ds(row, height), lane_slice] if first else there
        return pltpu.make_async_remote_copy(
            src_ref=here,
            dst_ref=there,
            send_sem=ring_send.at[number, step],
            recv_sem=ring_recv.at[number, recv_step],
            device_id=((ahead, behind)[way], t),
            device_id_type=MESH,
        )

    lag, gap, late, conv_a, conv_b, wait_sum, wait_share = PLAN
    offsets = [
        layer * (last + gap) + extra
        for layer in range(layers)
        for extra in (0, min(late if layer == layers - 1 else lag, last))
    ]
    edges = sorted({offset + extra for offset in offsets for extra in (0, 1, last, last + 1)})
    clock = [0]

    def advance(to):
        while clock[0] < to:
            now = clock[0]
            end = min([edge for edge in edges if edge > now] + [to])
            end = min(end, to)
            active = [
                (stage, offset, now - offset)
                for stage, offset in zip(numbered, offsets)
                if 0 <= now - offset <= last
            ]

            def slot(at):
                for stage, offset, shown in active:
                    step = at - offset
                    for number, piece in stage:
                        if shown == 0:
                            ring_copy(number, piece, 0, True, 0).start()
                            continue
                        if shown == last:
                            which, layer, way, row, height, lane, lanes = piece
                            ring_copy(number, piece, last - 1, False, last - 1).wait_recv()
                            continue
                        ring_copy(number, piece, step, False, step - 1).wait_recv()
                        ring_copy(number, piece, step, False, step).start()

            if end - now == 1:
                slot(now)
            else:
                def body(at, carry):
                    slot(at)
                    return carry

                lax.fori_loop(now, end, body, 0)
            clock[0] = end

    def share_copy(layer, source, mask, sub):
        return pltpu.make_async_remote_copy(
            src_ref=source,
            dst_ref=gathered.at[layer, partner(sub)],
            send_sem=x_send.at[layer, mask ^ sub],
            recv_sem=x_recv.at[layer, mask ^ sub],
            device_id=(s, partner(mask)),
            device_id_type=MESH,
        )

    order = [(mask, sub) for place_, mask in enumerate(masks) for sub in span(masks[:place_])]

    def share_start(layer, source):
        for mask in masks:
            share_copy(layer, source, mask, 0).start()
        gathered[layer, t] = source[...]

    def share_relay(layer, source):
        for mask, sub in order:
            if sub:
                got = gathered.at[layer, partner(sub)]
                share_copy(layer, got, mask, sub).start()
            share_copy(layer, source, mask, sub).wait_recv()

    def share_end(layer, source):
        for mask, sub in order:
            share_copy(layer, source, mask, sub).wait_send()

    def normalise(layer):
        squares = jnp.zeros((tokens, 1), F32)
        for block in range(peers):
            value = gathered[layer, block].astype(F32)
            squares += jnp.sum(value * value, axis=1, keepdims=True)
        scale = lax.rsqrt(squares / features + 1e-06)
        for block in range(peers):
            gain = gain_ref[layer : layer + 1, block * part : (block + 1) * part]
            normed[:, block * part : (block + 1) * part] = (
                gathered[layer, block].astype(F32) * scale * gain
            ).astype(BF16)

    def halo_copy(layer):
        return pltpu.make_async_remote_copy(
            src_ref=glu.at[layer, pl.ds(tokens - taps, taps), :],
            dst_ref=halo.at[layer],
            send_sem=halo_send.at[layer],
            recv_sem=halo_recv.at[layer],
            device_id=(after, t),
            device_id_type=MESH,
        )

    def gated(layer):
        value = jnp.dot(normed[...], full[0, layer], preferred_element_type=F32)
        gate = jnp.dot(normed[...], full[1, layer], preferred_element_type=F32)
        rounded = (value * jax.nn.sigmoid(gate)).astype(BF16)
        glu[layer] = rounded

        @pl.when(s < last)
        def _():
            halo_copy(layer).start()

        wide = rounded.astype(F32)
        for group in range(groups):
            padded[group, taps:, :] = wide[:, group * LANES : (group + 1) * LANES]

    def halo_arrive(layer):
        @pl.when(s > 0)
        def _():
            halo_copy(layer).wait_recv()
            wide = halo[layer].astype(F32)
            for group in range(groups):
                padded[group, :taps, :] = wide[:, group * LANES : (group + 1) * LANES]

        @pl.when(s == 0)
        def _():
            padded[:, :taps, :] = jnp.zeros((groups, taps, LANES), F32)

    half = tokens // 2

    def convolve(layer, which):
        for group in range(groups):
            lanes = slice(group * LANES, (group + 1) * LANES)

            def body(block, total, group=group, lanes=lanes):
                eight = taps_ref[layer, pl.ds(pl.multiple_of(block * 8, 8), 8), lanes]
                for unit in range(8):
                    total += eight[unit : unit + 1] * padded[group, pl.ds(which * half + block * 8 + unit + 1, half), :]
                return total

            conv[which * half : (which + 1) * half, lanes] = lax.fori_loop(
                0, taps // 8, body, jnp.zeros((half, LANES), F32)
            )

    def stat_copy(layer, bits):
        return pltpu.make_async_remote_copy(
            src_ref=stat.at[layer, t],
            dst_ref=stat.at[layer, t],
            send_sem=stat_send.at[layer, bits],
            recv_sem=stat_recv.at[layer, bits],
            device_id=(s, partner(bits)),
            device_id_type=MESH,
        )

    def stat_start(layer):
        value = conv[...]
        sums = jnp.sum(value, axis=1, keepdims=True)
        centred = value - sums / width
        squares = jnp.sum(centred * centred, axis=1, keepdims=True)
        lane = lax.broadcasted_iota(jnp.int32, (tokens, LANES), 1)
        packed = jnp.where(lane == 0, sums, jnp.where(lane == 1, squares, 0.0))
        stat[layer, t] = packed.T[:8, :]
        for bits in range(1, peers):
            stat_copy(layer, bits).start()

    def activate(layer):
        for bits in range(1, peers):
            stat_copy(layer, bits).wait_recv()
        every = [stat[layer, block] for block in range(peers)]
        mean = sum(entry[0:1] for entry in every) / channels
        squares = sum(
            entry[1:2] + width * (entry[0:1] / width - mean) * (entry[0:1] / width - mean) for entry in every
        )
        scale = lax.rsqrt(squares / channels + 1e-05)
        row = lax.broadcasted_iota(jnp.int32, (LANES, tokens), 0)
        columns = jnp.where(row == 0, mean, jnp.where(row == 1, scale, 0.0)).T
        v = (conv[...] - columns[:, 0:1]) * columns[:, 1:2] * channel_ref[layer : layer + 1, :]
        act[...] = (v * jax.nn.sigmoid(v)).astype(BF16)

    def sum_copy(layer, mask, sub):
        return pltpu.make_async_remote_copy(
            src_ref=leaving.at[layer, mask ^ sub],
            dst_ref=landing.at[layer, mask ^ sub],
            send_sem=sum_send.at[layer, mask ^ sub],
            recv_sem=sum_recv.at[layer, mask ^ sub],
            device_id=(s, partner(mask)),
            device_id_type=MESH,
        )

    rising = masks[::-1]

    upright = wo_ref.shape[1] == width and wo_ref.shape[2] % LANES == 0
    owned = count // peers

    def product(layer, bits):
        whose = partner(bits)
        if upright:
            found = [
                jnp.dot(act[...], full_out[layer, whose * owned + block], preferred_element_type=F32)
                for block in range(owned)
            ]
            return jnp.concatenate(found, axis=1)
        found = full_out[layer, pl.ds(whose * owned, owned)].reshape(part, width)
        return lax.dot_general(act[...], found, (((1,), (1,)), ((), ())), preferred_element_type=F32)

    def reduce_start(layer):
        mask = rising[0]
        subs = span(rising[1:])[::-1]
        for sub in subs:
            leaving[layer, mask ^ sub] = product(layer, mask ^ sub).astype(BF16)
            sum_copy(layer, mask, sub).start()
        for sub in subs:
            mine[sub] = product(layer, sub)
            sum_copy(layer, mask, sub).wait_recv()
            mine[sub] = mine[sub] + landing[layer, mask ^ sub].astype(F32)
            if len(rising) > 1 and sub & rising[1]:
                leaving[layer, sub] = mine[sub].astype(BF16)
                sum_copy(layer, rising[1], sub ^ rising[1]).start()

    def reduce_end(layer, source, target):
        for level in range(1, len(rising)):
            mask = rising[level]
            for sub in span(rising[level + 1 :])[::-1]:
                sum_copy(layer, mask, sub).wait_recv()
                mine[sub] = mine[sub] + landing[layer, mask ^ sub].astype(F32)
                if level + 1 < len(rising) and sub & rising[level + 1]:
                    leaving[layer, sub] = mine[sub].astype(BF16)
                    sum_copy(layer, rising[level + 1], sub ^ rising[level + 1]).start()
        target[...] = (source[...].astype(F32) + mine[0]).astype(BF16)

    current = x_ref
    share_start(0, current)
    advance(min(3, last))
    share_relay(0, current)
    advance(min(4, last))
    normalise(0)
    for layer in range(layers):
        base = offsets[2 * layer] + last
        if layer == 0:
            for own in own_copies:
                own.wait()
        advance(base + 1)
        gated(layer)
        advance(base + 1 + conv_a)
        halo_arrive(layer)
        convolve(layer, 0)
        advance(base + 1 + conv_b)
        convolve(layer, 1)
        stat_start(layer)
        advance(offsets[2 * layer + 1] + last + 1)
        activate(layer)
        reduce_start(layer)
        if layer + 1 < layers:
            advance(clock[0] + wait_sum)
            reduce_end(layer, current, middle.at[layer])
            current = middle.at[layer]
            share_start(layer + 1, current)
            advance(clock[0] + wait_share)
            share_relay(layer + 1, current)
            normalise(layer + 1)
        else:
            reduce_end(layer, current, out_ref)

    for layer in range(layers):
        source = x_ref if layer == 0 else middle.at[layer - 1]
        share_end(layer, source)
        for bits in range(1, peers):
            stat_copy(layer, bits).wait_send()
        for level, mask in enumerate(rising):
            for sub in span(rising[level + 1 :]):
                sum_copy(layer, mask, sub).wait_send()

        @pl.when(s < last)
        def _(layer=layer):
            halo_copy(layer).wait_send()

    def drain(step, carry):
        for stage in numbered:
            for number, piece in stage:
                ring_copy(number, piece, step, False, step).wait_send()
        return carry

    lax.fori_loop(0, last, drain, 0)


def shards(count, peers, stream, norm_gain, w_value, w_gate, conv_taps, channel_gain, w_out):
    tokens, part = stream.shape
    layers, rows, width = w_value.shape
    taps = conv_taps.shape[1]
    features = rows * count
    columns = w_out.shape[2]
    stages = ring_chunks(layers, rows, width, columns)
    outward = w_out if columns % LANES == 0 else jnp.swapaxes(w_out, 1, 2)
    pieces = sum(len(stage) for stage in stages)
    dma = pltpu.SemaphoreType.DMA
    return pl.pallas_call(
        functools.partial(kernel, count, peers, stages),
        out_shape=jax.ShapeDtypeStruct((tokens, part), BF16),
        in_specs=[pl.BlockSpec(memory_space=pltpu.VMEM)] * 7,
        out_specs=pl.BlockSpec(memory_space=pltpu.VMEM),
        scratch_shapes=[
            pltpu.VMEM((2, layers, features, width), BF16),
            pltpu.VMEM((layers, count, *outward.shape[1:]), BF16),
            pltpu.VMEM((layers, peers, tokens, part), BF16),
            pltpu.VMEM((tokens, features), BF16),
            pltpu.VMEM((layers, tokens, width), BF16),
            pltpu.VMEM((layers, taps, width), BF16),
            pltpu.VMEM((width // LANES, taps + tokens, LANES), F32),
            pltpu.VMEM((tokens, width), F32),
            pltpu.VMEM((layers, peers, 8, tokens), F32),
            pltpu.VMEM((tokens, width), BF16),
            pltpu.VMEM((peers, tokens, part), F32),
            pltpu.VMEM((layers, peers, tokens, part), BF16),
            pltpu.VMEM((layers, peers, tokens, part), BF16),
            pltpu.VMEM((layers, tokens, part), BF16),
            dma((pieces, count - 1)),
            dma((pieces, count - 1)),
            dma((layers, peers)),
            dma((layers, peers)),
            dma((layers,)),
            dma((layers,)),
            dma((layers, peers)),
            dma((layers, peers)),
            dma((layers, peers)),
            dma((layers, peers)),
            dma((3,)),
        ],
        compiler_params=pltpu.CompilerParams(
            collective_id=0, has_side_effects=True, vmem_limit_bytes=60 * 1024 * 1024
        ),
    )(stream, norm_gain, w_value, w_gate, conv_taps, channel_gain, outward)


def solution(mesh):
    return jax.shard_map(
        functools.partial(shards, mesh.shape["sp"], mesh.shape["tp"]),
        mesh=mesh,
        in_specs=(
            P("sp", "tp"),
            P(),
            P(None, "sp", "tp"),
            P(None, "sp", "tp"),
            P(None, None, "tp"),
            P(None, "tp"),
            P(None, "tp", "sp"),
        ),
        out_specs=P("sp", "tp"),
        check_vma=False,
    )
```

```python
import functools

import jax
import jax.numpy as jnp
from jax import lax
from jax.experimental import pallas as pl
from jax.experimental.pallas import tpu as pltpu
from jax.sharding import PartitionSpec as P

F32, BF16 = jnp.float32, jnp.bfloat16
LANES = 128
ROW_TILE = 16
MESH = pl.DeviceIdType.MESH
PLAN = (3, 0, 3, 1, 2, 2, 1)


def span(masks):
    found = [0]
    for mask in masks:
        found = found + [entry ^ mask for entry in found]
    return found


def parts_of(rows, most):
    parts = most
    while rows % (parts * ROW_TILE):
        parts //= 2
    return parts


def ring_chunks(layers, rows, width, columns):
    stages = []
    for layer in range(layers):
        parts = parts_of(rows, 4)
        step = rows // parts
        stages.append(
            [(which, layer, which, part * step, step, 0, width) for part in range(parts) for which in (0, 1)]
        )
        parts = parts_of(width, 4) if columns % LANES == 0 else 2
        high, step = (width // parts, columns) if columns % LANES == 0 else (rows, width // parts)
        stages.append(
            [
                (2, layer, part % 2, part * high, high, 0, step)
                if columns % LANES == 0
                else (2, layer, part % 2, 0, high, part * step, step)
                for part in range(parts)
            ]
        )
    return stages


def kernel(
    count, peers, stages,
    x_ref, gain_ref, wv_ref, wg_ref, taps_ref, channel_ref, wo_ref, out_ref,
    full, full_out, gathered, normed, glu, halo, padded, conv, stat, act, mine, leaving, landing, middle,
    ring_send, ring_recv, x_send, x_recv, halo_send, halo_recv, stat_send, stat_recv, sum_send, sum_recv, own_sem,
):
    s, t = lax.axis_index("sp"), lax.axis_index("tp")
    tokens, part = x_ref.shape
    layers, rows, width = wv_ref.shape
    features = rows * count
    taps = taps_ref.shape[1]
    channels = width * peers
    groups = width // LANES
    last = count - 1

    odd = s % 2
    place = (1 - odd) * (s // 2) + odd * (last - s // 2)

    def at_place(where):
        where = (where + count) % count
        upper = where // (count // 2)
        return (1 - upper) * (2 * where) + upper * (2 * (last - where) + 1)

    ahead, behind = at_place(place + 1), at_place(place - 1)
    masks = []
    mask = peers // 2
    while mask:
        masks.append(mask)
        mask //= 2

    def partner(bits):
        other = t
        for mask in masks:
            if bits & mask:
                other = other + mask - 2 * mask * ((t // mask) % 2)
        return other

    after, before = (s + 1) % count, (s + last) % count
    barrier = pltpu.get_barrier_semaphore()
    greeted = [(ahead, t), (behind, t), (after, t), (before, t)]
    greeted += [(s, partner(bits)) for bits in range(1, peers)]
    for who in greeted:
        pl.semaphore_signal(barrier, inc=1, device_id=who, device_id_type=MESH)
    pl.semaphore_wait(barrier, len(greeted))

    sources = (wv_ref, wg_ref, wo_ref)
    own_copies = []
    for which in range(3):
        own_place = full.at[which, :, pl.ds(pl.multiple_of(s * rows, rows), rows), :] if which < 2 else full_out.at[:, s]
        own = pltpu.make_async_copy(sources[which], own_place, own_sem.at[which])
        own.start()
        own_copies.append(own)

    numbered, total = [], 0
    for stage in stages:
        numbered.append([(total + offset, piece) for offset, piece in enumerate(stage)])
        total += len(stage)

    def ring_copy(number, piece, step, first, recv_step):
        which, layer, way, row, height, lane, lanes = piece
        block = at_place(place - step) if way == 0 else at_place(place + step)
        lane_slice = pl.ds(lane, lanes)
        if which < 2:
            start = pl.multiple_of(block * rows + row, ROW_TILE)
            there = full.at[which, layer, pl.ds(start, height), lane_slice]
        else:
            there = full_out.at[layer, block, pl.ds(row, height), lane_slice]
        here = sources[which].at[layer, pl.ds(row, height), lane_slice] if first else there
        return pltpu.make_async_remote_copy(
            src_ref=here,
            dst_ref=there,
            send_sem=ring_send.at[number, step],
            recv_sem=ring_recv.at[number, recv_step],
            device_id=((ahead, behind)[way], t),
            device_id_type=MESH,
        )

    lag, gap, late, conv_a, conv_b, wait_sum, wait_share = PLAN
    offsets = [
        layer * (last + gap) + extra
        for layer in range(layers)
        for extra in (0, min(late if layer == layers - 1 else lag, last))
    ]
    edges = sorted({offset + extra for offset in offsets for extra in (0, 1, last, last + 1)})
    clock = [0]

    def advance(to):
        while clock[0] < to:
            now = clock[0]
            end = min([edge for edge in edges if edge > now] + [to])
            end = min(end, to)
            active = [
                (stage, offset, now - offset)
                for stage, offset in zip(numbered, offsets)
                if 0 <= now - offset <= last
            ]

            def slot(at):
                for stage, offset, shown in active:
                    step = at - offset
                    for number, piece in stage:
                        if shown == 0:
                            ring_copy(number, piece, 0, True, 0).start()
                            continue
                        if shown == last:
                            which, layer, way, row, height, lane, lanes = piece
                            ring_copy(number, piece, last - 1, False, last - 1).wait_recv()
                            continue
                        ring_copy(number, piece, step, False, step - 1).wait_recv()
                        ring_copy(number, piece, step, False, step).start()

            if end - now == 1:
                slot(now)
            else:
                def body(at, carry):
                    slot(at)
                    return carry

                lax.fori_loop(now, end, body, 0)
            clock[0] = end

    def share_copy(layer, source, mask, sub):
        return pltpu.make_async_remote_copy(
            src_ref=source,
            dst_ref=gathered.at[layer, partner(sub)],
            send_sem=x_send.at[layer, mask ^ sub],
            recv_sem=x_recv.at[layer, mask ^ sub],
            device_id=(s, partner(mask)),
            device_id_type=MESH,
        )

    order = [(mask, sub) for place_, mask in enumerate(masks) for sub in span(masks[:place_])]

    def share_start(layer, source):
        for mask in masks:
            share_copy(layer, source, mask, 0).start()
        gathered[layer, t] = source[...]

    def share_relay(layer, source):
        for mask, sub in order:
            if sub:
                got = gathered.at[layer, partner(sub)]
                share_copy(layer, got, mask, sub).start()
            share_copy(layer, source, mask, sub).wait_recv()

    def share_end(layer, source):
        for mask, sub in order:
            share_copy(layer, source, mask, sub).wait_send()

    def normalise(layer):
        squares = jnp.zeros((tokens, 1), F32)
        for block in range(peers):
            value = gathered[layer, block].astype(F32)
            squares += jnp.sum(value * value, axis=1, keepdims=True)
        scale = lax.rsqrt(squares / features + 1e-06)
        for block in range(peers):
            gain = gain_ref[layer : layer + 1, block * part : (block + 1) * part]
            normed[:, block * part : (block + 1) * part] = (
                gathered[layer, block].astype(F32) * scale * gain
            ).astype(BF16)

    def halo_copy(layer):
        return pltpu.make_async_remote_copy(
            src_ref=glu.at[layer, pl.ds(tokens - taps, taps), :],
            dst_ref=halo.at[layer],
            send_sem=halo_send.at[layer],
            recv_sem=halo_recv.at[layer],
            device_id=(after, t),
            device_id_type=MESH,
        )

    def gated(layer):
        value = jnp.dot(normed[...], full[0, layer], preferred_element_type=F32)
        gate = jnp.dot(normed[...], full[1, layer], preferred_element_type=F32)
        rounded = (value * jax.nn.sigmoid(gate)).astype(BF16)
        glu[layer] = rounded

        @pl.when(s < last)
        def _():
            halo_copy(layer).start()

        wide = rounded.astype(F32)
        for group in range(groups):
            padded[group, taps:, :] = wide[:, group * LANES : (group + 1) * LANES]

    def halo_arrive(layer):
        @pl.when(s > 0)
        def _():
            halo_copy(layer).wait_recv()
            wide = halo[layer].astype(F32)
            for group in range(groups):
                padded[group, :taps, :] = wide[:, group * LANES : (group + 1) * LANES]

        @pl.when(s == 0)
        def _():
            padded[:, :taps, :] = jnp.zeros((groups, taps, LANES), F32)

    half = tokens // 2

    def convolve(layer, which):
        for group in range(groups):
            lanes = slice(group * LANES, (group + 1) * LANES)

            def body(block, total, group=group, lanes=lanes):
                eight = taps_ref[layer, pl.ds(pl.multiple_of(block * 8, 8), 8), lanes]
                for unit in range(8):
                    total += eight[unit : unit + 1] * padded[group, pl.ds(which * half + block * 8 + unit + 1, half), :]
                return total

            conv[which * half : (which + 1) * half, lanes] = lax.fori_loop(
                0, taps // 8, body, jnp.zeros((half, LANES), F32)
            )

    def stat_copy(layer, bits):
        return pltpu.make_async_remote_copy(
            src_ref=stat.at[layer, t],
            dst_ref=stat.at[layer, t],
            send_sem=stat_send.at[layer, bits],
            recv_sem=stat_recv.at[layer, bits],
            device_id=(s, partner(bits)),
            device_id_type=MESH,
        )

    def stat_start(layer):
        value = conv[...]
        sums = jnp.sum(value, axis=1, keepdims=True)
        centred = value - sums / width
        squares = jnp.sum(centred * centred, axis=1, keepdims=True)
        lane = lax.broadcasted_iota(jnp.int32, (tokens, LANES), 1)
        packed = jnp.where(lane == 0, sums, jnp.where(lane == 1, squares, 0.0))
        stat[layer, t] = packed.T[:8, :]
        for bits in range(1, peers):
            stat_copy(layer, bits).start()

    def activate(layer):
        for bits in range(1, peers):
            stat_copy(layer, bits).wait_recv()
        every = [stat[layer, block] for block in range(peers)]
        mean = sum(entry[0:1] for entry in every) / channels
        squares = sum(
            entry[1:2] + width * (entry[0:1] / width - mean) * (entry[0:1] / width - mean) for entry in every
        )
        scale = lax.rsqrt(squares / channels + 1e-05)
        row = lax.broadcasted_iota(jnp.int32, (LANES, tokens), 0)
        columns = jnp.where(row == 0, mean, jnp.where(row == 1, scale, 0.0)).T
        v = (conv[...] - columns[:, 0:1]) * columns[:, 1:2] * channel_ref[layer : layer + 1, :]
        act[...] = (v * jax.nn.sigmoid(v)).astype(BF16)

    def sum_copy(layer, mask, sub):
        return pltpu.make_async_remote_copy(
            src_ref=leaving.at[layer, mask ^ sub],
            dst_ref=landing.at[layer, mask ^ sub],
            send_sem=sum_send.at[layer, mask ^ sub],
            recv_sem=sum_recv.at[layer, mask ^ sub],
            device_id=(s, partner(mask)),
            device_id_type=MESH,
        )

    rising = masks[::-1]

    upright = wo_ref.shape[1] == width and wo_ref.shape[2] % LANES == 0
    owned = count // peers

    def product(layer, bits):
        whose = partner(bits)
        if upright:
            found = [
                jnp.dot(act[...], full_out[layer, whose * owned + block], preferred_element_type=F32)
                for block in range(owned)
            ]
            return jnp.concatenate(found, axis=1)
        found = full_out[layer, pl.ds(whose * owned, owned)].reshape(part, width)
        return lax.dot_general(act[...], found, (((1,), (1,)), ((), ())), preferred_element_type=F32)

    def reduce_start(layer):
        mask = rising[0]
        subs = span(rising[1:])[::-1]
        for sub in subs:
            leaving[layer, mask ^ sub] = product(layer, mask ^ sub).astype(BF16)
            sum_copy(layer, mask, sub).start()
        for sub in subs:
            mine[sub] = product(layer, sub)
            sum_copy(layer, mask, sub).wait_recv()
            mine[sub] = mine[sub] + landing[layer, mask ^ sub].astype(F32)
            if len(rising) > 1 and sub & rising[1]:
                leaving[layer, sub] = mine[sub].astype(BF16)
                sum_copy(layer, rising[1], sub ^ rising[1]).start()

    def reduce_end(layer, source, target):
        for level in range(1, len(rising)):
            mask = rising[level]
            for sub in span(rising[level + 1 :])[::-1]:
                sum_copy(layer, mask, sub).wait_recv()
                mine[sub] = mine[sub] + landing[layer, mask ^ sub].astype(F32)
                if level + 1 < len(rising) and sub & rising[level + 1]:
                    leaving[layer, sub] = mine[sub].astype(BF16)
                    sum_copy(layer, rising[level + 1], sub ^ rising[level + 1]).start()
        target[...] = (source[...].astype(F32) + mine[0]).astype(BF16)

    joined = len(rising) == 2
    near, high = rising[0], rising[-1]

    def cross_copy(layer, sub):
        return pltpu.make_async_remote_copy(
            src_ref=leaving.at[layer, sub],
            dst_ref=landing.at[layer, sub ^ high],
            send_sem=sum_send.at[layer, sub],
            recv_sem=sum_recv.at[layer, sub ^ high],
            device_id=(s, partner(high)),
            device_id_type=MESH,
        )

    def spread_start(layer):
        for sub in (high, 0):
            leaving[layer, near ^ sub] = product(layer, near ^ sub).astype(BF16)
            sum_copy(layer, near, sub).start()
        for sub in (high, 0):
            own_part = product(layer, sub)
            sum_copy(layer, near, sub).wait_recv()
            leaving[layer, sub] = (own_part + landing[layer, near ^ sub].astype(F32)).astype(BF16)
            cross_copy(layer, sub).start()

    def spread_end(layer, sub):
        cross_copy(layer, sub ^ high).wait_recv()
        whose = partner(sub)
        both = leaving[layer, sub].astype(F32) + landing[layer, sub].astype(F32)
        gathered[layer + 1, whose] = (gathered[layer, whose].astype(F32) + both).astype(BF16)
        share_copy(layer + 1, gathered.at[layer + 1, whose], near, sub).start()

    current = x_ref
    share_start(0, current)
    advance(min(5, last))
    share_relay(0, current)
    advance(min(6, last))
    normalise(0)
    for layer in range(layers):
        base = offsets[2 * layer] + last
        if layer == 0:
            for own in own_copies:
                own.wait()
        advance(base + 1)
        gated(layer)
        advance(base + 1 + conv_a)
        halo_arrive(layer)
        convolve(layer, 0)
        advance(base + 1 + conv_b)
        convolve(layer, 1)
        stat_start(layer)
        advance(offsets[2 * layer + 1] + last + 1)
        activate(layer)
        if joined and layer + 1 < layers:
            spread_start(layer)
            advance(clock[0] + wait_sum)
            spread_end(layer, 0)
            advance(clock[0] + wait_share)
            spread_end(layer, high)
            for sub in (0, high):
                share_copy(layer + 1, gathered.at[layer + 1, t], near, sub).wait_recv()
            normalise(layer + 1)
            current = gathered.at[layer + 1, t]
            continue
        reduce_start(layer)
        if layer + 1 < layers:
            advance(clock[0] + wait_sum)
            reduce_end(layer, current, middle.at[layer])
            current = middle.at[layer]
            share_start(layer + 1, current)
            advance(clock[0] + wait_share)
            share_relay(layer + 1, current)
            normalise(layer + 1)
        else:
            reduce_end(layer, current, out_ref)

    for layer in range(layers):
        source = x_ref if layer == 0 else middle.at[layer - 1]
        if joined and layer:
            for sub in (0, high):
                share_copy(layer, gathered.at[layer, t], near, sub).wait_send()
        else:
            share_end(layer, source)
        for bits in range(1, peers):
            stat_copy(layer, bits).wait_send()
        for level, mask in enumerate(rising):
            for sub in span(rising[level + 1 :]):
                if joined and layer + 1 < layers and level:
                    cross_copy(layer, 0).wait_send()
                    cross_copy(layer, high).wait_send()
                else:
                    sum_copy(layer, mask, sub).wait_send()

        @pl.when(s < last)
        def _(layer=layer):
            halo_copy(layer).wait_send()

    def drain(step, carry):
        for stage in numbered:
            for number, piece in stage:
                ring_copy(number, piece, step, False, step).wait_send()
        return carry

    lax.fori_loop(0, last, drain, 0)


def shards(count, peers, stream, norm_gain, w_value, w_gate, conv_taps, channel_gain, w_out):
    tokens, part = stream.shape
    layers, rows, width = w_value.shape
    taps = conv_taps.shape[1]
    features = rows * count
    columns = w_out.shape[2]
    stages = ring_chunks(layers, rows, width, columns)
    outward = w_out if columns % LANES == 0 else jnp.swapaxes(w_out, 1, 2)
    pieces = sum(len(stage) for stage in stages)
    dma = pltpu.SemaphoreType.DMA
    return pl.pallas_call(
        functools.partial(kernel, count, peers, stages),
        out_shape=jax.ShapeDtypeStruct((tokens, part), BF16),
        in_specs=[pl.BlockSpec(memory_space=pltpu.VMEM)] * 7,
        out_specs=pl.BlockSpec(memory_space=pltpu.VMEM),
        scratch_shapes=[
            pltpu.VMEM((2, layers, features, width), BF16),
            pltpu.VMEM((layers, count, *outward.shape[1:]), BF16),
            pltpu.VMEM((layers, peers, tokens, part), BF16),
            pltpu.VMEM((tokens, features), BF16),
            pltpu.VMEM((layers, tokens, width), BF16),
            pltpu.VMEM((layers, taps, width), BF16),
            pltpu.VMEM((width // LANES, taps + tokens, LANES), F32),
            pltpu.VMEM((tokens, width), F32),
            pltpu.VMEM((layers, peers, 8, tokens), F32),
            pltpu.VMEM((tokens, width), BF16),
            pltpu.VMEM((peers, tokens, part), F32),
            pltpu.VMEM((layers, peers, tokens, part), BF16),
            pltpu.VMEM((layers, peers, tokens, part), BF16),
            pltpu.VMEM((layers, tokens, part), BF16),
            dma((pieces, count - 1)),
            dma((pieces, count - 1)),
            dma((layers, peers)),
            dma((layers, peers)),
            dma((layers,)),
            dma((layers,)),
            dma((layers, peers)),
            dma((layers, peers)),
            dma((layers, peers)),
            dma((layers, peers)),
            dma((3,)),
        ],
        compiler_params=pltpu.CompilerParams(
            collective_id=0, has_side_effects=True, vmem_limit_bytes=60 * 1024 * 1024
        ),
    )(stream, norm_gain, w_value, w_gate, conv_taps, channel_gain, outward)


def solution(mesh):
    return jax.shard_map(
        functools.partial(shards, mesh.shape["sp"], mesh.shape["tp"]),
        mesh=mesh,
        in_specs=(
            P("sp", "tp"),
            P(),
            P(None, "sp", "tp"),
            P(None, "sp", "tp"),
            P(None, None, "tp"),
            P(None, "tp"),
            P(None, "tp", "sp"),
        ),
        out_specs=P("sp", "tp"),
        check_vma=False,
    )
```
